32 devices in a mesh: ep: 8 (over z, core), tp: 4 (over y, x).
Axes of the slice: x: 2, y: 2, z: 4, core: 2. Of those that a mesh axis runs over, the one named last changes fastest.
Arguments:
- queries: bfloat16 [2048, 4096], P('ep', 'tp'), may hold values from -6 to 6
- keys: bfloat16 [2048, 1024], P('ep', 'tp'), may hold values from -6 to 6
- values: bfloat16 [2048, 1024], P('ep', 'tp'), may hold values from -6 to 6
- query_gain: float32 [64], replicated, may hold values from 1 to 11
- key_gain: float32 [64], replicated, may hold values from 1 to 11
- moe_rows: bfloat16 [2048, 4096], P('ep', 'tp'), may hold values from -14 to 14
- route_ids: int32 [2048, 2], P('ep'), may hold values from 0 to 7, all different within a row; in each aligned block of 256 rows (0 to 255, 256 to 511, ...) at most 96 rows name the same one
- group_weight: float32 [2048], P('ep'), may hold values from 0.2 to 1
- expert_weight: float32 [2048, 2], P('ep'), may hold values from 0.05 to 1
- expert_gate: bfloat16 [8, 4096, 2048], P('ep', None, 'tp'), may hold values from -0.09375 to 0.09375
- expert_up: bfloat16 [8, 4096, 2048], P('ep', None, 'tp'), may hold values from -0.09375 to 0.09375
- expert_down: bfloat16 [8, 2048, 4096], P('ep', None, 'tp'), may hold values from -0.125 to 0.125
Outputs:
- attended: bfloat16 [2048, 4096], P('ep', 'tp')
- moe_out: bfloat16 [2048, 4096], P('ep', 'tp')
The draws below stay inside these ranges and needn't reach their ends.
Inputs may be any that keep to these rules, and one draw needn't show every extreme that they name: `route_ids`: each row names 2 different experts. Among the rows of one device no expert is named by more than 96 rows, and in every draw some expert is named by exactly 96 of them.
All inputs are finite; a program needn't handle non-finite values.
Results may differ from the reference program's by a relative error of at most 0.0055.
The reference program's roundings to bfloat16 on the way count: a program that leaves them out, or rounds other values in their place, can miss the bound.
Values may be sent and summed in bfloat16 or wider, within the bound.
A program may use at most 128 MiB of HBM per device.

```python
import math
import jax
import jax.numpy as jnp
import numpy as np
from jax import lax

D = 4096
HEAD_DIM = 64
HEADS = 64
KV_HEADS = 16
FF = 2048
GRID_W = 64
TOPK = 2
TOK_DEV = 256
TOKENS = 2048
EXPERTS = 8
CAP = 96
N_EP = 8


def query_key_pair(key):
    folded = jax.random.fold_in(key, 17)
    key_one, key_two = jax.random.split(folded, 2)
    query_draw = jnp.clip(jax.random.normal(key_one, (TOKENS, HEADS * HEAD_DIM), jnp.float32), -6.0, 6.0)
    key_draw = jnp.clip(jax.random.normal(key_two, (TOKENS, KV_HEADS * HEAD_DIM), jnp.float32), -6.0, 6.0)
    return (query_draw, key_draw)


def draw_queries(key, part):
    return query_key_pair(key)[0].astype(jnp.bfloat16)


def draw_keys(key, part):
    return query_key_pair(key)[1].astype(jnp.bfloat16)


def gain_draw(key, salt):
    folded = jax.random.fold_in(key, salt)
    spread = 1.5 * jnp.exp(jax.random.uniform(folded, (HEAD_DIM,), jnp.float32, -0.3, 0.3))
    return spread


def draw_query_gain(key, part):
    return gain_draw(key, 31)


def draw_key_gain(key, part):
    return gain_draw(key, 37)


def draw_moe_rows(key, part):
    folded = jax.random.fold_in(key, 23)
    key_one, key_two = jax.random.split(folded)
    base_part = jnp.clip(jax.random.normal(key_one, (TOKENS, D), jnp.float32), -4.0, 4.0)
    scales = jnp.exp(jax.random.uniform(key_two, (TOKENS, 1), jnp.float32, -1.2, 1.2))
    return (base_part * scales).astype(jnp.bfloat16)


def steps_of(rng, extent, cuts, least, top_value):
    factor_of = 1.0
    for dim, parts in cuts:
        heights = jax.random.uniform(jax.random.fold_in(jax.random.fold_in(rng, 6), dim), (parts,), jnp.float32, least / len(cuts), top_value / len(cuts))
        factor_of = factor_of * jnp.repeat(jnp.exp(heights), extent[dim] // parts).reshape((-1,) + (1,) * (len(extent) - 1 - dim))
    return factor_of


def assign_block(stream_key, own, number, rows, count, top, bound, slope):
    sequence = jax.random.permutation(stream_key, count)
    crowded, ordinary = load_shares(count, rows * top, bound, slope, True), load_shares(count, rows * top, bound, slope, False)
    places = jnp.arange(count)

    def named(lengths, offset_by):
        used = int((lengths > 0).sum())
        fixed = max(1, used // 4)
        moved = fixed + (places - fixed + offset_by * (used - fixed)) % max(1, count - fixed)
        return jnp.zeros((count,), jnp.int32).at[sequence[jnp.where(places < fixed, places, moved)]].set(jnp.asarray(lengths, jnp.int32))

    lengths = jnp.where(number % 4 == 0, named(crowded, number // 4), named(ordinary, number - number // 4 - 1))
    mixed = jax.random.permutation(jax.random.fold_in(own, 3), count)
    source_of, taker = mixed[0:count // 2 * 2:2], mixed[1:count // 2 * 2:2]
    margin = jnp.minimum(lengths[source_of] - 1, bound - lengths[taker]) // 2
    margin = jnp.where((source_of == sequence[0]) | (taker == sequence[0]) | (lengths[taker] == 0), 0, jnp.maximum(margin, 0))
    moved = jax.random.randint(jax.random.fold_in(own, 4), (count // 2,), 0, 1 << 20) % (margin + 1)
    lengths = lengths.at[source_of].add(-moved).at[taker].add(moved)
    labels = jnp.searchsorted(jnp.cumsum(lengths), jnp.arange(rows * top), side="right").astype(jnp.int32)
    table = labels.reshape(top, rows).T
    table = table[jax.random.permutation(jax.random.fold_in(own, 1), rows)]
    offset_by = jax.random.randint(jax.random.fold_in(own, 2), (rows, 1), 0, top)
    return jnp.take_along_axis(table, (jnp.arange(top)[None, :] + offset_by) % top, axis=1)


def load_shares(amount, total, bound, skew, full):
    portions = [(1 << 20) // math.isqrt(grade ** skew) + 1 for grade in range(1, amount + 1)]
    largest = bound if full else min(bound, max(-(-total // amount), total * portions[0] // sum(portions)))
    least = 1 if total - largest >= amount - 1 else 0
    counts, spare = [largest] + [least] * (amount - 1), total - largest - least * (amount - 1)
    while spare > 0:
        candidates = [i for i in range(1, amount) if counts[i] < largest] or [i for i in range(1, amount) if counts[i] < bound]
        whole, remaining = sum([portions[i] for i in candidates]), spare
        for i in candidates:
            addition = min(bound - counts[i], max(1, remaining * portions[i] // whole), spare)
            counts[i] = counts[i] + addition
            spare = spare - addition
    return np.array(counts)


def normal_values(own_key, dims, deviation, bound, cuts=(), kind=jnp.bfloat16):
    entries = deviation * jax.random.normal(own_key, dims, jnp.float32)
    if cuts:
        entries = entries * steps_of(own_key, dims, cuts, -0.22, 0.18)
    return jnp.clip(entries, -bound, bound).astype(kind)


def setup_inputs(seed: int = 0) -> dict:
    key_of = jax.random.split(jax.random.key(seed), 13)
    queries = draw_queries(jax.random.fold_in(key_of[12], 71), 0)
    keys = draw_keys(jax.random.fold_in(key_of[12], 71), 0)
    values = normal_values(key_of[2], (TOKENS, KV_HEADS * HEAD_DIM), 1.0, 6.0, ((0, 8), (1, 4)))
    query_gain = draw_query_gain(jax.random.fold_in(key_of[12], 71), 0)
    key_gain = draw_key_gain(jax.random.fold_in(key_of[12], 71), 0)
    moe_rows = draw_moe_rows(jax.random.fold_in(key_of[12], 71), 0)
    route_ids_keys = jax.random.split(jax.random.fold_in(key_of[6], 1), TOKENS // TOK_DEV)
    route_ids_turns = jax.random.permutation(jax.random.fold_in(key_of[6], 3), TOKENS // TOK_DEV)
    route_ids = jax.vmap(lambda own, number: assign_block(jax.random.fold_in(key_of[6], 2), own, number, TOK_DEV, EXPERTS, TOPK, CAP, 1))(route_ids_keys, route_ids_turns).reshape((TOKENS, TOPK))
    group_weight = jnp.clip(jnp.exp(math.log(1.0) - 1.609438 * jax.random.uniform(key_of[7], (TOKENS,), jnp.float32) ** steps_of(key_of[7], (TOKENS,), ((0, 8),), -0.2, 0.2)), 0.2, 1.0)
    expert_weight = jnp.clip(jnp.exp(math.log(1.0) - 2.9957323 * jax.random.uniform(key_of[8], (TOKENS, TOPK), jnp.float32) ** steps_of(key_of[8], (TOKENS, TOPK), ((0, 8),), -0.2, 0.2)), 0.05, 1.0)
    expert_gate = normal_values(key_of[9], (EXPERTS, D, FF), D ** -0.5, 0.09375, ((0, 8), (2, 4)))
    expert_up = normal_values(key_of[10], (EXPERTS, D, FF), D ** -0.5, 0.09375, ((0, 8), (2, 4)))
    expert_down = normal_values(key_of[11], (EXPERTS, FF, D), FF ** -0.5, 0.125, ((0, 8), (2, 4)))
    return dict(queries=queries, keys=keys, values=values, query_gain=query_gain, key_gain=key_gain, moe_rows=moe_rows, route_ids=route_ids, group_weight=group_weight, expert_weight=expert_weight, expert_gate=expert_gate, expert_up=expert_up, expert_down=expert_down)


def rotary_tables(position):
    pair_count = HEAD_DIM // 4
    grid_pos = jnp.stack([position // GRID_W, position % GRID_W], axis=-1).astype(jnp.float32)
    frequency = 10000.0 ** (-jnp.arange(pair_count, dtype=jnp.float32) / pair_count)
    angles = grid_pos[:, :, None] * frequency
    return (jnp.cos(angles), jnp.sin(angles))

def normed_rotated(rows_in, gain, cosine, sine_of):
    row_count, head_count = (rows_in.shape[0], rows_in.shape[1])
    pair_count = HEAD_DIM // 4
    scaled = rows_in * lax.rsqrt(lax.optimization_barrier(jnp.mean(rows_in * rows_in, axis=-1, keepdims=True)) + 1e-06) * gain
    parted = scaled.reshape(row_count, head_count, 2, 2, pair_count)
    first_half, second = (parted[:, :, :, 0, :], parted[:, :, :, 1, :])
    cos_b, sin_b = (cosine[:, None], sine_of[:, None])
    turned = jnp.stack([first_half * cos_b - second * sin_b, second * cos_b + first_half * sin_b], axis=3)
    return turned.reshape(row_count, head_count, HEAD_DIM).astype(jnp.bfloat16)

def attend_reference(queries, keys, values, query_gain, key_gain):
    group_size = HEADS // KV_HEADS
    cosine, sine_of = rotary_tables(jnp.arange(TOKENS, dtype=jnp.int32))
    query_rot = normed_rotated(queries.astype(jnp.float32).reshape(TOKENS, HEADS, HEAD_DIM), query_gain, cosine, sine_of)
    key_rot = normed_rotated(keys.astype(jnp.float32).reshape(TOKENS, KV_HEADS, HEAD_DIM), key_gain, cosine, sine_of)
    value_heads = values.reshape(TOKENS, KV_HEADS, HEAD_DIM)
    block_rows = math.gcd(TOKENS, 512)
    query_heads = query_rot.reshape(TOKENS // block_rows, block_rows, KV_HEADS, group_size, HEAD_DIM).transpose(2, 0, 1, 3, 4)

    def one_head(inputs):
        q_part, k_head, v_head = inputs

        def one_block(q_blk):
            scores = jnp.einsum('qgd,sd->gqs', q_blk.astype(jnp.float32), k_head.astype(jnp.float32)) * HEAD_DIM ** (-0.5)
            weights = jnp.exp(scores - lax.optimization_barrier(jnp.max(scores, axis=-1, keepdims=True)))
            denominator = lax.optimization_barrier(jnp.sum(weights, axis=-1))
            low_weights = lax.optimization_barrier(weights.astype(jnp.bfloat16)).astype(jnp.float32)
            mixed_out = jnp.einsum('gqs,sd->qgd', low_weights, v_head.astype(jnp.float32))
            return (mixed_out / denominator.T[:, :, None]).astype(jnp.bfloat16)
        return lax.map(one_block, q_part)
    output = lax.map(one_head, (query_heads, key_rot.transpose(1, 0, 2), value_heads.transpose(1, 0, 2)))
    return output.transpose(1, 2, 0, 3, 4).reshape(TOKENS, HEADS * HEAD_DIM)

def experts_reference(moe_rows, route_ids, group_weight, expert_weight, expert_gate, expert_up, expert_down):
    picks = TOK_DEV * TOPK
    route_list = route_ids.reshape(N_EP, picks)
    one_hot = (route_list[:, :, None] == jnp.arange(EXPERTS, dtype=jnp.int32)[None, None, :]).astype(jnp.int32)
    rank_of = lax.optimization_barrier(jnp.sum((jnp.cumsum(one_hot, axis=1) - one_hot) * one_hot, axis=-1))
    source = jnp.arange(N_EP, dtype=jnp.int32)[:, None]
    slot_of = route_list * (N_EP * CAP) + source * CAP + rank_of
    owner_of = source * TOK_DEV + jnp.arange(picks, dtype=jnp.int32)[None, :] // TOPK
    slot_owner = jnp.full((EXPERTS * N_EP * CAP,), TOKENS, jnp.int32).at[slot_of.reshape(-1)].set(owner_of.reshape(-1))
    padded = jnp.concatenate([moe_rows, jnp.zeros((1, D), moe_rows.dtype)], axis=0)
    routed = padded[slot_owner].reshape(EXPERTS, N_EP * CAP, D)

    def one_expert(inputs):
        rows_in, w_gate, w_up, w_down = inputs
        widened = rows_in.astype(jnp.float32)
        inv_rms = lax.rsqrt(lax.optimization_barrier(jnp.mean(widened * widened, axis=-1, keepdims=True)) + 1e-06)
        gate_act = jnp.dot(rows_in, w_gate, preferred_element_type=jnp.float32) * inv_rms
        up_act = jnp.dot(rows_in, w_up, preferred_element_type=jnp.float32) * inv_rms
        hidden = (jax.nn.silu(gate_act) * up_act).astype(jnp.bfloat16)
        return jnp.dot(hidden, w_down, preferred_element_type=jnp.float32).astype(jnp.bfloat16)
    results = lax.map(one_expert, (routed, expert_gate, expert_up, expert_down)).reshape(EXPERTS * N_EP * CAP, D)
    picked = results[slot_of.reshape(TOKENS, TOPK)].astype(jnp.float32)
    mixing = group_weight[:, None] * expert_weight / lax.optimization_barrier(jnp.sum(expert_weight, axis=-1, keepdims=True))
    return lax.optimization_barrier(jnp.sum(mixing[:, :, None] * picked, axis=1)).astype(jnp.bfloat16)

def reference(queries, keys, values, query_gain, key_gain, moe_rows, route_ids, group_weight, expert_weight, expert_gate, expert_up, expert_down):
    attended = attend_reference(queries, keys, values, query_gain, key_gain)
    moe_out = experts_reference(moe_rows, route_ids, group_weight, expert_weight, expert_gate, expert_up, expert_down)
    return (attended, moe_out)
```

```python
import jax
import jax.numpy as jnp
import numpy as np
from jax import lax
from jax.experimental import pallas as pl
from jax.experimental.pallas import tpu as pltpu
from jax.sharding import PartitionSpec as P

D = 4096
HEAD_DIM = 64
GRID_W = 64
TOPK = 2


def rotary_tables(position):
    pair_count = HEAD_DIM // 4
    grid_pos = jnp.stack([position // GRID_W, position % GRID_W], axis=-1).astype(jnp.float32)
    frequency = 10000.0 ** (-jnp.arange(pair_count, dtype=jnp.float32) / pair_count)
    angles = grid_pos[:, :, None] * frequency
    return (jnp.cos(angles), jnp.sin(angles))


def normed_rotated(rows_in, gain, cosine, sine_of):
    row_count, head_count = (rows_in.shape[0], rows_in.shape[1])
    pair_count = HEAD_DIM // 4
    scaled = rows_in * lax.rsqrt(jnp.mean(rows_in * rows_in, axis=-1, keepdims=True) + 1e-06) * gain
    parted = scaled.reshape(row_count, head_count, 2, 2, pair_count)
    first_half, second = (parted[:, :, :, 0, :], parted[:, :, :, 1, :])
    cos_b, sin_b = (cosine[:, None], sine_of[:, None])
    turned = jnp.stack(
        [first_half * cos_b - second * sin_b, second * cos_b + first_half * sin_b], axis=3
    )
    return turned.reshape(row_count, head_count, HEAD_DIM).astype(jnp.bfloat16)


def attend_block(carried, portion, query_rot, kv_width):
    running_max, denominator, summed = carried
    key_count = portion.shape[0]
    head_count = kv_width // HEAD_DIM
    keys_part = portion[:, :kv_width].reshape(key_count, head_count, HEAD_DIM)
    values_part = portion[:, kv_width:].reshape(key_count, head_count, HEAD_DIM)
    scores = jnp.einsum(
        "tkgd,skd->kgts", query_rot, keys_part, preferred_element_type=jnp.float32
    ) * HEAD_DIM ** (-0.5)
    new_max = jnp.max(scores, axis=-1)
    factor = jnp.exp(running_max - new_max)
    weights = jnp.exp(scores - new_max[..., None])
    denominator = denominator * factor + jnp.sum(weights, axis=-1)
    summed = summed * factor[..., None] + jnp.einsum(
        "kgts,skd->kgtd",
        weights.astype(jnp.bfloat16),
        values_part,
        preferred_element_type=jnp.float32,
    )
    return (new_max, denominator, summed)


def plain_on_device(
    queries,
    keys,
    values,
    query_gain,
    key_gain,
    moe_rows,
    route_ids,
    group_weight,
    expert_weight,
    expert_gate,
    expert_up,
    expert_down,
):
    tok_rows = queries.shape[0]
    q_heads = queries.shape[1] // HEAD_DIM
    k_heads = keys.shape[1] // HEAD_DIM
    group_size = q_heads // k_heads
    position = lax.axis_index("ep") * tok_rows + jnp.arange(tok_rows, dtype=jnp.int32)
    cosine, sine_of = rotary_tables(position)
    query_rot = normed_rotated(
        queries.astype(jnp.float32).reshape(tok_rows, q_heads, HEAD_DIM),
        query_gain,
        cosine,
        sine_of,
    )
    query_rot = query_rot.reshape(tok_rows, k_heads, group_size, HEAD_DIM)
    key_rot = normed_rotated(
        keys.astype(jnp.float32).reshape(tok_rows, k_heads, HEAD_DIM), key_gain, cosine, sine_of
    )
    kv_width = k_heads * HEAD_DIM
    joined = jnp.concatenate([key_rot.reshape(tok_rows, kv_width), values], axis=1)
    initial = (
        jnp.full((k_heads, group_size, tok_rows), -jnp.inf, jnp.float32),
        jnp.zeros((k_heads, group_size, tok_rows), jnp.float32),
        jnp.zeros((k_heads, group_size, tok_rows, HEAD_DIM), jnp.float32),
    )
    final_max, denominator, summed = attend_block(
        initial, lax.all_gather(joined, "ep", axis=0, tiled=True), query_rot, kv_width
    )
    attended = (
        (summed / denominator[..., None])
        .transpose(2, 0, 1, 3)
        .reshape(tok_rows, q_heads * HEAD_DIM)
        .astype(jnp.bfloat16)
    )
    moe_tokens = moe_rows.shape[0]
    local_experts = expert_gate.shape[0]
    expert_count = local_experts * lax.axis_size("ep")
    capacity = 3 * moe_tokens * TOPK // (2 * expert_count)
    picks = moe_tokens * TOPK
    route_list = route_ids.reshape(picks)
    one_hot = (route_list[:, None] == jnp.arange(expert_count, dtype=jnp.int32)[None, :]).astype(
        jnp.int32
    )
    rank_of = jnp.sum((jnp.cumsum(one_hot, axis=0) - one_hot) * one_hot, axis=1)
    slot_of = route_list * capacity + rank_of
    owner_of = (
        jnp.full((expert_count * capacity,), moe_tokens, jnp.int32)
        .at[slot_of]
        .set(jnp.arange(picks, dtype=jnp.int32) // TOPK)
    )
    padded = jnp.concatenate([moe_rows, jnp.zeros((1, moe_rows.shape[1]), moe_rows.dtype)], axis=0)
    arrived = lax.all_to_all(
        padded[owner_of].reshape(expert_count, capacity, moe_rows.shape[1]),
        "ep",
        split_axis=0,
        concat_axis=1,
        tiled=True,
    )
    portion = lax.all_gather(arrived, "tp", axis=2, tiled=True)
    widened = portion.astype(jnp.float32)
    gate_act = jnp.einsum("erd,edf->erf", portion, expert_gate, preferred_element_type=jnp.float32)
    up_act = jnp.einsum("erd,edf->erf", portion, expert_up, preferred_element_type=jnp.float32)
    square_sum = jnp.sum(widened * widened, axis=2)
    inv_rms = lax.rsqrt(square_sum / D + 1e-06)[..., None]
    hidden = (jax.nn.silu(gate_act * inv_rms) * (up_act * inv_rms)).astype(jnp.bfloat16)
    out_cols = expert_down.shape[2]
    expert_result = jnp.einsum(
        "erf,efd->erd",
        lax.all_gather(hidden, "tp", axis=2, tiled=True),
        expert_down,
        preferred_element_type=jnp.float32,
    ).astype(jnp.bfloat16)
    returned = lax.all_to_all(expert_result, "ep", split_axis=1, concat_axis=0, tiled=True)
    flat_back = returned.reshape(expert_count * capacity, out_cols)
    picked = flat_back[slot_of].reshape(moe_tokens, TOPK, out_cols).astype(jnp.float32)
    mixing = group_weight[:, None] * expert_weight / jnp.sum(expert_weight, axis=1, keepdims=True)
    moe_out = jnp.sum(mixing[:, :, None] * picked, axis=1).astype(jnp.bfloat16)
    return (attended, moe_out)


MESH = pl.DeviceIdType.MESH


def flip(index, mask, width):
    out = 0
    bit = 1
    while bit < width:
        a, b = (index // bit) % 2, (mask // bit) % 2
        out = out + bit * (a + b - 2 * a * b)
        bit *= 2
    return out


def sub_iota(shape):
    return lax.broadcasted_iota(jnp.int32, shape, 0)


def lane_iota(shape):
    return lax.broadcasted_iota(jnp.int32, shape, 1)


def main_kernel(
    ep, cap,
    qg_ref, kg_ref, rowtab, coltab, route_ref, gw_ref, ew_ref,
    rows_hbm, k_hbm, v_hbm, q_hbm, wg_hbm, wu_hbm, wd_hbm,
    att_hbm, moe_hbm,
    rows_v, k_v, v_v, q_v, code_ref, pick0, pick1, mix_ref, picks,
    xg, hid, res, ret, kvall, q_s, cos_ref, sin_ref, acc, att_v, moe_v, wg, wu, wd,
    l_sem, o_sem, d_send, d_recv, x_send, x_recv, xr_send, xr_recv,
    h_send, h_recv, hr_send, hr_recv, r_send, r_recv, k_send, k_recv,
):
    me, tme = lax.axis_index("ep"), lax.axis_index("tp")
    sides = (flip(tme, 1, 4), flip(tme, 2, 4))
    half = cap // 2
    width = wg.shape[1]
    tok, chan = rows_v.shape
    f32, bf = jnp.float32, jnp.bfloat16

    def mask(p):
        if isinstance(p, int):
            return 0 if p == 0 else p % (ep - 1) + 1
        return jnp.where(p == 0, 0, p % (ep - 1) + 1)

    def peer(p):
        return flip(me, mask(p), ep)

    pairs = (
        (rows_hbm, rows_v), (k_hbm, k_v), (v_hbm, v_v), (q_hbm, q_v),
        (wg_hbm.at[0], wg), (wu_hbm.at[0], wu), (wd_hbm.at[0], wd),
    )
    loads = [pltpu.make_async_copy(a, b, l_sem.at[n]) for n, (a, b) in enumerate(pairs)]
    for copy in loads:
        copy.start()
    barrier = pltpu.get_barrier_semaphore()
    for j in range(1, ep):
        pl.semaphore_signal(barrier, inc=1, device_id={"ep": flip(me, j, ep)}, device_id_type=MESH)
    for side in sides:
        pl.semaphore_signal(barrier, inc=1, device_id={"tp": side}, device_id_type=MESH)

    def remote(src, dst, send, recv, device):
        return pltpu.make_async_remote_copy(
            src_ref=src, dst_ref=dst, send_sem=send, recv_sem=recv,
            device_id=device, device_id_type=MESH,
        )

    def dispatch(p):
        return remote(picks.at[p], xg.at[p, tme], d_send.at[p], d_recv.at[p], {"ep": peer(p)})

    def keys_out(j):
        return remote(
            kvall.at[me], kvall.at[me], k_send.at[j], k_recv.at[j], {"ep": flip(me, j, ep)}
        )

    def keys_on(j, to):
        block = flip(me, j, ep)
        n = flip(j, to, ep)
        return remote(
            kvall.at[block], kvall.at[block], k_send.at[n], k_recv.at[n],
            {"ep": flip(me, to, ep)},
        )

    def cross(p, n):
        part = xg.at[p, tme]
        return remote(part, part, x_send.at[p, n], x_recv.at[p, n], {"tp": sides[n]})

    def cross_on(p, n):
        part = xg.at[p, sides[n], pl.ds(n * half, half)]
        return remote(part, part, xr_send.at[p, n], xr_recv.at[p, n], {"tp": sides[1 - n]})

    def wide(p, n):
        part = hid.at[p, tme]
        return remote(part, part, h_send.at[p, n], h_recv.at[p, n], {"tp": sides[n]})

    def wide_on(p, n):
        part = hid.at[p, sides[n], pl.ds(n * half, half)]
        return remote(part, part, hr_send.at[p, n], hr_recv.at[p, n], {"tp": sides[1 - n]})

    def back(p):
        return remote(res.at[p], ret.at[p], r_send.at[p], r_recv.at[p], {"ep": peer(p)})

    experts = sub_iota((16, tok))
    first = route_ref[0:1, :] == experts
    second = route_ref[1:2, :] == experts
    both = jnp.logical_or(first, second)
    earlier = jnp.where(sub_iota((tok, tok)) < lane_iota((tok, tok)), 1.0, 0.0).astype(bf)
    rank = jnp.dot(
        jnp.where(both, 1.0, 0.0).astype(bf), earlier, preferred_element_type=f32
    )
    code = jnp.where(both, rank, -1.0)
    for e in range(ep):
        code_ref[e] = code[e : e + 1, :]
    slots = sub_iota((cap, tok)).astype(f32)

    def select(p):
        chosen = jnp.where(code_ref[peer(p)] == slots, 1.0, 0.0).astype(bf)
        return jnp.dot(chosen, rows_v[...], preferred_element_type=f32).astype(bf)

    loads[0].wait()
    xg[0, tme] = select(0)
    picks[1] = select(1)
    pl.semaphore_wait(barrier, ep + 1)
    for n in range(2):
        cross(0, n).start()
    dispatch(1).start()
    for p in range(2, 5):
        picks[p] = select(p)
        dispatch(p).start()

    spread = jnp.where(
        sub_iota((128, 128)) // HEAD_DIM == lane_iota((128, 128)) // HEAD_DIM, 1.0 / HEAD_DIM, 0.0
    ).astype(f32)
    grid_rows = tok // GRID_W
    for g in range(grid_rows):
        line = rowtab[me * grid_rows + g]
        cos_ref[g * GRID_W : (g + 1) * GRID_W, :] = line[:, :128] + coltab[:, :128]
        sin_ref[g * GRID_W : (g + 1) * GRID_W, :] = line[:, 128:] + coltab[:, 128:]
    lane = lane_iota((tok, 128))
    half_one = lane % 32 < 16
    low = lane < HEAD_DIM

    def turned(x, gain):
        x = x.astype(f32)
        mean = jnp.dot(
            x * x, spread, preferred_element_type=f32, precision=lax.Precision.HIGHEST
        )
        y = x * lax.rsqrt(mean + 1e-06) * gain
        partner = jnp.where(half_one, pltpu.roll(y, 112, 1), pltpu.roll(y, 16, 1))
        return y * cos_ref[...] + partner * sin_ref[...]

    q_gain = jnp.concatenate([qg_ref[...], qg_ref[...]], axis=1)
    k_gain = jnp.concatenate([kg_ref[...], kg_ref[...]], axis=1)
    k_slabs = k_v.shape[1] // 128
    slabs = q_v.shape[1] // 128
    per_kv = slabs // (2 * k_slabs)
    loads[1].wait()
    loads[2].wait()
    for s in range(k_slabs):
        kvall[me, s] = turned(k_v[:, s * 128 : (s + 1) * 128], k_gain).astype(bf)
        kvall[me, k_slabs + s] = v_v[:, s * 128 : (s + 1) * 128]
    picks[5] = select(5)
    for j in (1, 2, 4):
        keys_out(j).start()
    for p in range(5, ep):
        if p > 5:
            picks[p] = select(p)
        dispatch(p).start()

    loads[3].wait()
    for s in range(slabs):
        r = turned(q_v[:, s * 128 : (s + 1) * 128], q_gain)
        r = r.astype(bf).astype(f32) * HEAD_DIM ** (-0.5)
        moved = pltpu.roll(r, HEAD_DIM, 1)
        if (s // per_kv) % 2 == 0:
            pair = (jnp.where(low, r, 0.0), jnp.where(low, moved, 0.0))
        else:
            pair = (jnp.where(low, 0.0, moved), jnp.where(low, 0.0, r))
        q_s[2 * s] = pair[0].astype(bf)
        q_s[2 * s + 1] = pair[1].astype(bf)

    columns = lane_iota((16, ep * cap))
    place = jnp.zeros((16, ep * cap), jnp.int32)
    for n in range(1, ep):
        place = place + jnp.where(columns >= n * cap, 1, 0)
    xor_of = jnp.where(place == 0, 0, jnp.where(place == ep - 1, 1, place + 1))
    named = jnp.where(sub_iota((16, ep * cap)) == jnp.bitwise_xor(xor_of, me), 1.0, 0.0).astype(bf)
    rest = (columns - place * cap).astype(f32)[0:1, :]
    for wanted, out in ((first, pick0), (second, pick1)):
        of_token = jnp.where(wanted, rank, -1.0).T.astype(bf)
        spot = jnp.dot(of_token, named, preferred_element_type=f32)
        out[...] = jnp.where(spot == rest, 1.0, 0.0).astype(bf)
    weight = gw_ref[...] * ew_ref[...] / jnp.sum(ew_ref[...], axis=0, keepdims=True)
    mix_ref[...] = jnp.concatenate([weight, jnp.zeros((6, tok), f32)], axis=0).T

    def enter(p):
        dispatch(p).wait_recv()
        for n in range(2):
            cross(p, n).start()

    def relay(p):
        for n in range(2):
            cross(p, n).wait_recv()
            cross_on(p, n).start()

    enter(1)
    relay(0)
    enter(2)
    relay(1)
    for copy in loads[4:]:
        copy.wait()

    def first_half(p):
        for n in range(2):
            cross_on(p, n).wait_recv()
        gate = jnp.zeros((cap, width), f32)
        up = jnp.zeros((cap, width), f32)
        square = jnp.zeros((cap, 1), f32)
        for a in range(4):
            x = xg[p, a]
            w = x.astype(f32)
            square = square + jnp.sum(w * w, axis=1, keepdims=True)
            gate = gate + jnp.dot(x, wg[a * chan : (a + 1) * chan, :], preferred_element_type=f32)
            up = up + jnp.dot(x, wu[a * chan : (a + 1) * chan, :], preferred_element_type=f32)
        inv = lax.rsqrt(square / D + 1e-06)
        g = gate * inv
        hid[p, tme] = (g / (1.0 + jnp.exp(-g)) * (up * inv)).astype(bf)
        for n in range(2):
            wide(p, n).start()

    def second_half(p):
        for n in range(2):
            wide_on(p, n).wait_recv()
        total = jnp.zeros((cap, chan), f32)
        for a in range(4):
            total = total + jnp.dot(
                hid[p, a], wd[a * width : (a + 1) * width, :], preferred_element_type=f32
            )
        return total.astype(bf)

    keys_total = ep * tok

    def attend(m, carry):
        pp = m // (2 * per_kv)
        k = kvall[:, pp].reshape(keys_total, 128)
        v = kvall[:, k_slabs + pp].reshape(keys_total, 128)
        outs = []
        for d in range(2):
            s = lax.dot_general(
                q_s[2 * m + d], k, (((1,), (1,)), ((), ())), preferred_element_type=f32
            )
            p = jnp.exp(s - jnp.max(s, axis=1, keepdims=True))
            den = jnp.sum(p, axis=1, keepdims=True)
            o = jnp.dot(p.astype(bf), v, preferred_element_type=f32)
            outs.append(o / den)
        even = jnp.where(low, outs[0], pltpu.roll(outs[1], HEAD_DIM, 1))
        odd = jnp.where(low, pltpu.roll(outs[0], HEAD_DIM, 1), outs[1])
        side = ((m // per_kv) % 2).astype(f32)
        joined = jnp.where(side == 0.0, even, odd)
        att_v[:, pl.ds(pl.multiple_of(m * 128, 128), 128)] = joined.astype(bf)
        return carry

    def step(i, carry):
        first_half(i)

        @pl.when(i < ep - 3)
        def _():
            enter(i + 3)

        @pl.when(i < ep - 2)
        def _():
            relay(i + 2)

        @pl.when(i == 1)
        def _():
            ret[0] = second_half(0)

        @pl.when(i > 1)
        def _():
            res[i - 1] = second_half(i - 1)
            back(i - 1).start()

        @pl.when(i == KEYS_AT)
        def _():
            keys_out(2).wait_recv()
            keys_on(2, 1).start()
            keys_out(4).wait_recv()
            keys_on(4, 2).start()
            keys_on(4, 1).start()

        @pl.when(i == KEYS_AT + 1)
        def _():
            keys_on(4, 2).wait_recv()
            keys_on(6, 1).start()
            keys_out(1).wait_recv()
            for j in (2, 4, 6):
                keys_on(j, 1).wait_recv()

        begin = jnp.clip((i - UNITS_AT) * UNITS, 0, slabs)
        end = jnp.clip((i - UNITS_AT + 1) * UNITS, 0, slabs)
        lax.fori_loop(begin, end, attend, 0)
        for n in range(2):
            wide(i, n).wait_recv()
            wide_on(i, n).start()
        return carry

    lax.fori_loop(0, ep, step, 0)
    att_out = pltpu.make_async_copy(att_v, att_hbm, o_sem.at[0])
    att_out.start()

    def weighed(start, rows):
        block = ret[start : start + rows].reshape(rows * cap, chan)
        span = slice(start * cap, (start + rows) * cap)
        one = jnp.dot(pick0[:, span], block, preferred_element_type=f32)
        two = jnp.dot(pick1[:, span], block, preferred_element_type=f32)
        return mix_ref[:, 0:1] * one + mix_ref[:, 1:2] * two

    for p in range(1, ep - 2):
        back(p).wait_recv()
    acc[...] = weighed(0, ep - 2)
    res[ep - 1] = second_half(ep - 1)
    back(ep - 1).start()
    back(ep - 2).wait_recv()
    back(ep - 1).wait_recv()
    moe_v[...] = (acc[...] + weighed(ep - 2, 2)).astype(bf)
    moe_out = pltpu.make_async_copy(moe_v, moe_hbm, o_sem.at[1])
    moe_out.start()

    for p in range(ep):
        for n in range(2):
            cross(p, n).wait_send()
            cross_on(p, n).wait_send()
            wide(p, n).wait_send()
            wide_on(p, n).wait_send()
        if p > 0:
            dispatch(p).wait_send()
            back(p).wait_send()
    for j in (1, 2, 4):
        keys_out(j).wait_send()
    keys_on(4, 2).wait_send()
    for j in (2, 4, 6):
        keys_on(j, 1).wait_send()
    att_out.wait()
    moe_out.wait()


KEYS_AT = 2
UNITS_AT = 3
UNITS = 2


def angle_tables(lines):
    lane = np.arange(128)
    pair_count = HEAD_DIM // 4
    frequency = (10000.0 ** (-(lane % pair_count) / pair_count)).astype(np.float32)
    on_rows = (lane // (2 * pair_count)) % 2 == 0
    sign = np.where((lane // pair_count) % 2 == 0, -1.0, 1.0)

    def table(count, mine):
        angle = (np.arange(count, dtype=np.float32)[:, None] * frequency).astype(np.float64)
        both = np.concatenate(
            [np.cos(angle) * mine, np.sin(angle) * sign * mine], axis=1
        )
        return both.astype(np.float32)

    return table(lines, on_rows)[:, None, :], table(GRID_W, ~on_rows)


def on_device(
    queries, keys, values, query_gain, key_gain, moe_rows, route_ids, group_weight,
    expert_weight, expert_gate, expert_up, expert_down,
):
    ep, tp = lax.axis_size("ep"), lax.axis_size("tp")
    moe_tokens, chan = moe_rows.shape
    tok = queries.shape[0]
    cap = 3 * moe_tokens * TOPK // (2 * expert_gate.shape[0] * ep)
    fits = tp == 4 and ep == 8 and cap % 32 == 0 and expert_gate.shape[0] == 1
    fits = fits and tok == moe_tokens and tok % GRID_W == 0
    if not fits or queries.shape[1] // 128 != 8 or keys.shape[1] // 128 != 2:
        return plain_on_device(
            queries, keys, values, query_gain, key_gain, moe_rows, route_ids, group_weight,
            expert_weight, expert_gate, expert_up, expert_down,
        )
    rowtab, coltab = angle_tables(ep * tok // GRID_W)
    heads = queries.shape[1] // HEAD_DIM
    slabs = keys.shape[1] // 128
    width = expert_gate.shape[2]
    vmem = pl.BlockSpec(memory_space=pltpu.VMEM)
    hbm = pl.BlockSpec(memory_space=pl.ANY)
    dma = pltpu.SemaphoreType.DMA
    bf, f32 = jnp.bfloat16, jnp.float32
    attended, moe_out = pl.pallas_call(
        lambda *refs: main_kernel(ep, cap, *refs),
        out_shape=(
            jax.ShapeDtypeStruct(queries.shape, bf),
            jax.ShapeDtypeStruct(moe_rows.shape, bf),
        ),
        in_specs=[vmem] * 7 + [hbm] * 7,
        out_specs=(hbm, hbm),
        scratch_shapes=[
            pltpu.VMEM(moe_rows.shape, bf),
            pltpu.VMEM(keys.shape, bf),
            pltpu.VMEM(values.shape, bf),
            pltpu.VMEM(queries.shape, bf),
            pltpu.VMEM((ep, 1, tok), f32),
            pltpu.VMEM((tok, ep * cap), bf),
            pltpu.VMEM((tok, ep * cap), bf),
            pltpu.VMEM((tok, 8), f32),
            pltpu.VMEM((ep, cap, chan), bf),
            pltpu.VMEM((ep, tp, cap, chan), bf),
            pltpu.VMEM((ep, tp, cap, width), bf),
            pltpu.VMEM((ep, cap, chan), bf),
            pltpu.VMEM((ep, cap, chan), bf),
            pltpu.VMEM((ep, 2 * slabs, tok, 128), bf),
            pltpu.VMEM((heads, tok, 128), bf),
            pltpu.VMEM((tok, 128), f32),
            pltpu.VMEM((tok, 128), f32),
            pltpu.VMEM((tok, chan), f32),
            pltpu.VMEM(queries.shape, bf),
            pltpu.VMEM(moe_rows.shape, bf),
            pltpu.VMEM(expert_gate.shape[1:], bf),
            pltpu.VMEM(expert_up.shape[1:], bf),
            pltpu.VMEM(expert_down.shape[1:], bf),
            dma((7,)), dma((2,)), dma((ep,)), dma((ep,)),
            dma((ep, 2)), dma((ep, 2)), dma((ep, 2)), dma((ep, 2)),
            dma((ep, 2)), dma((ep, 2)), dma((ep, 2)), dma((ep, 2)),
            dma((ep,)), dma((ep,)), dma((ep,)), dma((ep,)),
        ],
        compiler_params=pltpu.CompilerParams(
            collective_id=0, has_side_effects=True, vmem_limit_bytes=60 * 1024 * 1024
        ),
    )(
        query_gain[None, :], key_gain[None, :], jnp.asarray(rowtab), jnp.asarray(coltab),
        route_ids.T, group_weight[None, :], expert_weight.T,
        moe_rows, keys, values, queries, expert_gate, expert_up, expert_down,
    )
    return (attended, moe_out)


def solution(mesh):
    placed = (
        P("ep", "tp"),
        P("ep", "tp"),
        P("ep", "tp"),
        P(),
        P(),
        P("ep", "tp"),
        P("ep", None),
        P("ep"),
        P("ep", None),
        P("ep", None, "tp"),
        P("ep", None, "tp"),
        P("ep", None, "tp"),
    )
    return jax.shard_map(
        on_device,
        mesh=mesh,
        in_specs=placed,
        out_specs=(P("ep", "tp"), P("ep", "tp")),
        check_vma=False,
    )
```

```python
import jax
import jax.numpy as jnp
import numpy as np
from jax import lax
from jax.experimental import pallas as pl
from jax.experimental.pallas import tpu as pltpu
from jax.sharding import PartitionSpec as P

D = 4096
HEAD_DIM = 64
GRID_W = 64
TOPK = 2


def rotary_tables(position):
    pair_count = HEAD_DIM // 4
    grid_pos = jnp.stack([position // GRID_W, position % GRID_W], axis=-1).astype(jnp.float32)
    frequency = 10000.0 ** (-jnp.arange(pair_count, dtype=jnp.float32) / pair_count)
    angles = grid_pos[:, :, None] * frequency
    return (jnp.cos(angles), jnp.sin(angles))


def normed_rotated(rows_in, gain, cosine, sine_of):
    row_count, head_count = (rows_in.shape[0], rows_in.shape[1])
    pair_count = HEAD_DIM // 4
    scaled = rows_in * lax.rsqrt(jnp.mean(rows_in * rows_in, axis=-1, keepdims=True) + 1e-06) * gain
    parted = scaled.reshape(row_count, head_count, 2, 2, pair_count)
    first_half, second = (parted[:, :, :, 0, :], parted[:, :, :, 1, :])
    cos_b, sin_b = (cosine[:, None], sine_of[:, None])
    turned = jnp.stack(
        [first_half * cos_b - second * sin_b, second * cos_b + first_half * sin_b], axis=3
    )
    return turned.reshape(row_count, head_count, HEAD_DIM).astype(jnp.bfloat16)


def attend_block(carried, portion, query_rot, kv_width):
    running_max, denominator, summed = carried
    key_count = portion.shape[0]
    head_count = kv_width // HEAD_DIM
    keys_part = portion[:, :kv_width].reshape(key_count, head_count, HEAD_DIM)
    values_part = portion[:, kv_width:].reshape(key_count, head_count, HEAD_DIM)
    scores = jnp.einsum(
        "tkgd,skd->kgts", query_rot, keys_part, preferred_element_type=jnp.float32
    ) * HEAD_DIM ** (-0.5)
    new_max = jnp.max(scores, axis=-1)
    factor = jnp.exp(running_max - new_max)
    weights = jnp.exp(scores - new_max[..., None])
    denominator = denominator * factor + jnp.sum(weights, axis=-1)
    summed = summed * factor[..., None] + jnp.einsum(
        "kgts,skd->kgtd",
        weights.astype(jnp.bfloat16),
        values_part,
        preferred_element_type=jnp.float32,
    )
    return (new_max, denominator, summed)


def plain_on_device(
    queries,
    keys,
    values,
    query_gain,
    key_gain,
    moe_rows,
    route_ids,
    group_weight,
    expert_weight,
    expert_gate,
    expert_up,
    expert_down,
):
    tok_rows = queries.shape[0]
    q_heads = queries.shape[1] // HEAD_DIM
    k_heads = keys.shape[1] // HEAD_DIM
    group_size = q_heads // k_heads
    position = lax.axis_index("ep") * tok_rows + jnp.arange(tok_rows, dtype=jnp.int32)
    cosine, sine_of = rotary_tables(position)
    query_rot = normed_rotated(
        queries.astype(jnp.float32).reshape(tok_rows, q_heads, HEAD_DIM),
        query_gain,
        cosine,
        sine_of,
    )
    query_rot = query_rot.reshape(tok_rows, k_heads, group_size, HEAD_DIM)
    key_rot = normed_rotated(
        keys.astype(jnp.float32).reshape(tok_rows, k_heads, HEAD_DIM), key_gain, cosine, sine_of
    )
    kv_width = k_heads * HEAD_DIM
    joined = jnp.concatenate([key_rot.reshape(tok_rows, kv_width), values], axis=1)
    initial = (
        jnp.full((k_heads, group_size, tok_rows), -jnp.inf, jnp.float32),
        jnp.zeros((k_heads, group_size, tok_rows), jnp.float32),
        jnp.zeros((k_heads, group_size, tok_rows, HEAD_DIM), jnp.float32),
    )
    final_max, denominator, summed = attend_block(
        initial, lax.all_gather(joined, "ep", axis=0, tiled=True), query_rot, kv_width
    )
    attended = (
        (summed / denominator[..., None])
        .transpose(2, 0, 1, 3)
        .reshape(tok_rows, q_heads * HEAD_DIM)
        .astype(jnp.bfloat16)
    )
    moe_tokens = moe_rows.shape[0]
    local_experts = expert_gate.shape[0]
    expert_count = local_experts * lax.axis_size("ep")
    capacity = 3 * moe_tokens * TOPK // (2 * expert_count)
    picks = moe_tokens * TOPK
    route_list = route_ids.reshape(picks)
    one_hot = (route_list[:, None] == jnp.arange(expert_count, dtype=jnp.int32)[None, :]).astype(
        jnp.int32
    )
    rank_of = jnp.sum((jnp.cumsum(one_hot, axis=0) - one_hot) * one_hot, axis=1)
    slot_of = route_list * capacity + rank_of
    owner_of = (
        jnp.full((expert_count * capacity,), moe_tokens, jnp.int32)
        .at[slot_of]
        .set(jnp.arange(picks, dtype=jnp.int32) // TOPK)
    )
    padded = jnp.concatenate([moe_rows, jnp.zeros((1, moe_rows.shape[1]), moe_rows.dtype)], axis=0)
    arrived = lax.all_to_all(
        padded[owner_of].reshape(expert_count, capacity, moe_rows.shape[1]),
        "ep",
        split_axis=0,
        concat_axis=1,
        tiled=True,
    )
    portion = lax.all_gather(arrived, "tp", axis=2, tiled=True)
    widened = portion.astype(jnp.float32)
    gate_act = jnp.einsum("erd,edf->erf", portion, expert_gate, preferred_element_type=jnp.float32)
    up_act = jnp.einsum("erd,edf->erf", portion, expert_up, preferred_element_type=jnp.float32)
    square_sum = jnp.sum(widened * widened, axis=2)
    inv_rms = lax.rsqrt(square_sum / D + 1e-06)[..., None]
    hidden = (jax.nn.silu(gate_act * inv_rms) * (up_act * inv_rms)).astype(jnp.bfloat16)
    out_cols = expert_down.shape[2]
    expert_result = jnp.einsum(
        "erf,efd->erd",
        lax.all_gather(hidden, "tp", axis=2, tiled=True),
        expert_down,
        preferred_element_type=jnp.float32,
    ).astype(jnp.bfloat16)
    returned = lax.all_to_all(expert_result, "ep", split_axis=1, concat_axis=0, tiled=True)
    flat_back = returned.reshape(expert_count * capacity, out_cols)
    picked = flat_back[slot_of].reshape(moe_tokens, TOPK, out_cols).astype(jnp.float32)
    mixing = group_weight[:, None] * expert_weight / jnp.sum(expert_weight, axis=1, keepdims=True)
    moe_out = jnp.sum(mixing[:, :, None] * picked, axis=1).astype(jnp.bfloat16)
    return (attended, moe_out)


MESH = pl.DeviceIdType.MESH


def flip(index, mask, width):
    out = 0
    bit = 1
    while bit < width:
        a, b = (index // bit) % 2, (mask // bit) % 2
        out = out + bit * (a + b - 2 * a * b)
        bit *= 2
    return out


def sub_iota(shape):
    return lax.broadcasted_iota(jnp.int32, shape, 0)


def lane_iota(shape):
    return lax.broadcasted_iota(jnp.int32, shape, 1)


def main_kernel(
    ep, cap,
    qg_ref, kg_ref, rowtab, coltab, route_ref, gw_ref, ew_ref,
    rows_hbm, k_hbm, v_hbm, q_hbm, wg_hbm, wu_hbm, wd_hbm,
    att_hbm, moe_hbm,
    rows_v, k_v, v_v, q_v, code_ref, pick0, pick1, mix_ref, picks,
    xg, hid, res, ret, kvall, q_s, tops, dens, part_o, cos_ref, sin_ref, acc, att_v, moe_v, wg, wu, wd,
    l_sem, o_sem, d_send, d_recv, x_send, x_recv, xr_send, xr_recv,
    h_send, h_recv, hr_send, hr_recv, r_send, r_recv, k_send, k_recv,
):
    me, tme = lax.axis_index("ep"), lax.axis_index("tp")
    sides = (flip(tme, 1, 4), flip(tme, 2, 4))
    half = cap // 2
    width = wg.shape[1]
    tok, chan = rows_v.shape
    f32, bf = jnp.float32, jnp.bfloat16
    order = (0, *range(2, ep), 1)

    def mask(p):
        if isinstance(p, int):
            return order[p]
        return jnp.where(p == 0, 0, p % (ep - 1) + 1)

    def peer(p):
        return flip(me, mask(p), ep)

    pairs = (
        (rows_hbm, rows_v), (k_hbm, k_v), (v_hbm, v_v), (q_hbm, q_v),
        (wg_hbm.at[0], wg), (wu_hbm.at[0], wu), (wd_hbm.at[0], wd),
    )
    loads = [pltpu.make_async_copy(a, b, l_sem.at[n]) for n, (a, b) in enumerate(pairs)]
    for copy in loads:
        copy.start()
    barrier = pltpu.get_barrier_semaphore()
    for j in range(1, ep):
        pl.semaphore_signal(barrier, inc=1, device_id={"ep": flip(me, j, ep)}, device_id_type=MESH)
    for side in sides:
        pl.semaphore_signal(barrier, inc=1, device_id={"tp": side}, device_id_type=MESH)

    def remote(src, dst, send, recv, device):
        return pltpu.make_async_remote_copy(
            src_ref=src, dst_ref=dst, send_sem=send, recv_sem=recv,
            device_id=device, device_id_type=MESH,
        )

    def dispatch(p):
        return remote(picks.at[p], xg.at[p, tme], d_send.at[p], d_recv.at[p], {"ep": peer(p)})

    def slot(b):
        return b // 2 % 2 * (ep // 2) + b // 4 * 2 + b % 2

    def keys_out(j):
        part = kvall.at[slot(me)]
        return remote(
            part, part, k_send.at[j], k_recv.at[j], {"ep": flip(me, j, ep)}
        )

    def keys_on(j, to):
        part = kvall.at[slot(flip(me, j, ep))]
        n = flip(j, to, ep)
        return remote(
            part, part, k_send.at[n], k_recv.at[n],
            {"ep": flip(me, to, ep)},
        )

    def cross(p, n):
        part = xg.at[p, tme]
        return remote(part, part, x_send.at[p, n], x_recv.at[p, n], {"tp": sides[n]})

    def cross_on(p, n):
        part = xg.at[p, sides[n], pl.ds(n * half, half)]
        return remote(part, part, xr_send.at[p, n], xr_recv.at[p, n], {"tp": sides[1 - n]})

    def wide(p, n):
        part = hid.at[p, tme]
        return remote(part, part, h_send.at[p, n], h_recv.at[p, n], {"tp": sides[n]})

    def wide_on(p, n):
        part = hid.at[p, sides[n], pl.ds(n * half, half)]
        return remote(part, part, hr_send.at[p, n], hr_recv.at[p, n], {"tp": sides[1 - n]})

    def back(p):
        return remote(res.at[p], ret.at[p], r_send.at[p], r_recv.at[p], {"ep": peer(p)})

    experts = sub_iota((16, tok))
    first = route_ref[0:1, :] == experts
    second = route_ref[1:2, :] == experts
    both = jnp.logical_or(first, second)
    earlier = jnp.where(sub_iota((tok, tok)) < lane_iota((tok, tok)), 1.0, 0.0).astype(bf)
    rank = jnp.dot(
        jnp.where(both, 1.0, 0.0).astype(bf), earlier, preferred_element_type=f32
    )
    code = jnp.where(both, rank, -1.0)
    for e in range(ep):
        code_ref[e] = code[e : e + 1, :]
    slots = sub_iota((cap, tok)).astype(f32)

    def select(p):
        chosen = jnp.where(code_ref[peer(p)] == slots, 1.0, 0.0).astype(bf)
        return jnp.dot(chosen, rows_v[...], preferred_element_type=f32).astype(bf)

    loads[0].wait()
    xg[0, tme] = select(0)
    picks[1] = select(1)
    pl.semaphore_wait(barrier, ep + 1)
    for n in range(2):
        cross(0, n).start()
    dispatch(1).start()
    picks[ep - 1] = select(ep - 1)
    dispatch(ep - 1).start()

    def enter(p):
        dispatch(p).wait_recv()
        for n in range(2):
            cross(p, n).start()

    def relay(p):
        for n in range(2):
            cross(p, n).wait_recv()
            cross_on(p, n).start()

    picks[2] = select(2)
    spread = jnp.where(
        sub_iota((128, 128)) // HEAD_DIM == lane_iota((128, 128)) // HEAD_DIM, 1.0 / HEAD_DIM, 0.0
    ).astype(f32)
    grid_rows = tok // GRID_W
    for g in range(grid_rows):
        line = rowtab[me * grid_rows + g]
        cos_ref[g * GRID_W : (g + 1) * GRID_W, :] = line[:, :128] + coltab[:, :128]
        sin_ref[g * GRID_W : (g + 1) * GRID_W, :] = line[:, 128:] + coltab[:, 128:]
    lane = lane_iota((tok, 128))
    half_one = lane % 32 < 16
    low = lane < HEAD_DIM

    def turned(x, gain):
        x = x.astype(f32)
        mean = jnp.dot(
            x * x, spread, preferred_element_type=f32, precision=lax.Precision.HIGHEST
        )
        y = x * lax.rsqrt(mean + 1e-06) * gain
        partner = jnp.where(half_one, pltpu.roll(y, 112, 1), pltpu.roll(y, 16, 1))
        return y * cos_ref[...] + partner * sin_ref[...]

    q_gain = jnp.concatenate([qg_ref[...], qg_ref[...]], axis=1)
    k_gain = jnp.concatenate([kg_ref[...], kg_ref[...]], axis=1)
    k_slabs = k_v.shape[1] // 128
    slabs = q_v.shape[1] // 128
    per_kv = slabs // (2 * k_slabs)
    loads[1].wait()
    loads[2].wait()
    for s in range(k_slabs):
        kvall[slot(me), s] = turned(k_v[:, s * 128 : (s + 1) * 128], k_gain).astype(bf)
        kvall[slot(me), k_slabs + s] = v_v[:, s * 128 : (s + 1) * 128]
    for j in (1, 4):
        keys_out(j).start()
    enter(ep - 1)
    for p in range(3, ep - 1):
        picks[p] = select(p)
    relay(0)
    dispatch(2).start()
    enter(1)
    relay(ep - 1)
    dispatch(3).start()

    loads[3].wait()
    for s in range(slabs):
        r = turned(q_v[:, s * 128 : (s + 1) * 128], q_gain)
        r = r.astype(bf).astype(f32) * HEAD_DIM ** (-0.5)
        moved = pltpu.roll(r, HEAD_DIM, 1)
        if (s // per_kv) % 2 == 0:
            pair = (jnp.where(low, r, 0.0), jnp.where(low, moved, 0.0))
        else:
            pair = (jnp.where(low, 0.0, moved), jnp.where(low, 0.0, r))
        q_s[2 * s] = pair[0].astype(bf)
        q_s[2 * s + 1] = pair[1].astype(bf)

    columns = lane_iota((16, ep * cap))
    place = jnp.zeros((16, ep * cap), jnp.int32)
    for n in range(1, ep):
        place = place + jnp.where(columns >= n * cap, 1, 0)
    xor_of = jnp.zeros((16, ep * cap), jnp.int32)
    for n in range(ep):
        xor_of = xor_of + jnp.where(place == n, order[n], 0)
    named = jnp.where(sub_iota((16, ep * cap)) == jnp.bitwise_xor(xor_of, me), 1.0, 0.0).astype(bf)
    rest = (columns - place * cap).astype(f32)[0:1, :]
    for wanted, out in ((first, pick0), (second, pick1)):
        of_token = jnp.where(wanted, rank, -1.0).T.astype(bf)
        spot = jnp.dot(of_token, named, preferred_element_type=f32)
        out[...] = jnp.where(spot == rest, 1.0, 0.0).astype(bf)
    weight = gw_ref[...] * ew_ref[...] / jnp.sum(ew_ref[...], axis=0, keepdims=True)
    mix_ref[...] = jnp.concatenate([weight, jnp.zeros((6, tok), f32)], axis=0).T

    keys_out(2).start()
    for copy in loads[4:]:
        copy.wait()

    def first_half(p):
        for n in range(2):
            cross_on(p, n).wait_recv()
        gate = jnp.zeros((cap, width), f32)
        up = jnp.zeros((cap, width), f32)
        square = jnp.zeros((cap, 1), f32)
        for a in range(4):
            x = xg[p, a]
            w = x.astype(f32)
            square = square + jnp.sum(w * w, axis=1, keepdims=True)
            gate = gate + jnp.dot(x, wg[a * chan : (a + 1) * chan, :], preferred_element_type=f32)
            up = up + jnp.dot(x, wu[a * chan : (a + 1) * chan, :], preferred_element_type=f32)
        inv = lax.rsqrt(square / D + 1e-06)
        g = gate * inv
        hid[p, tme] = (g / (1.0 + jnp.exp(-g)) * (up * inv)).astype(bf)

    def second_half(p):
        for n in range(2):
            wide_on(p, n).wait_recv()
        total = jnp.zeros((cap, chan), f32)
        for a in range(4):
            total = total + jnp.dot(
                hid[p, a], wd[a * width : (a + 1) * width, :], preferred_element_type=f32
            )
        return total.astype(bf)

    keys_total = ep * tok

    part_keys = keys_total // 2

    def scores(m, d, group):
        pp = m // (2 * per_kv)
        blocks = pl.ds(group * (ep // 2), ep // 2)
        k = kvall[blocks, pp].reshape(part_keys, 128)
        v = kvall[blocks, k_slabs + pp].reshape(part_keys, 128)
        s = lax.dot_general(
            q_s[2 * m + d], k, (((1,), (1,)), ((), ())), preferred_element_type=f32
        )
        return s, v

    def near(m, carry):
        for d in range(2):
            s, v = scores(m, d, me // 2 % 2)
            top = jnp.max(s, axis=1, keepdims=True)
            p = jnp.exp(s - top)
            tops[2 * m + d] = top
            dens[2 * m + d] = jnp.sum(p, axis=1, keepdims=True)
            part_o[2 * m + d] = jnp.dot(p.astype(bf), v, preferred_element_type=f32)
        return carry

    def far(m, carry):
        outs = []
        for d in range(2):
            s, v = scores(m, d, 1 - me // 2 % 2)
            before = tops[2 * m + d]
            top = jnp.maximum(before, jnp.max(s, axis=1, keepdims=True))
            scale = jnp.exp(before - top)
            p = jnp.exp(s - top)
            den = dens[2 * m + d] * scale + jnp.sum(p, axis=1, keepdims=True)
            o = part_o[2 * m + d] * scale + jnp.dot(p.astype(bf), v, preferred_element_type=f32)
            outs.append(o / den)
        even = jnp.where(low, outs[0], pltpu.roll(outs[1], HEAD_DIM, 1))
        odd = jnp.where(low, pltpu.roll(outs[0], HEAD_DIM, 1), outs[1])
        side = ((m // per_kv) % 2).astype(f32)
        joined = jnp.where(side == 0.0, even, odd)
        att_v[:, pl.ds(pl.multiple_of(m * 128, 128), 128)] = joined.astype(bf)
        return carry

    def attend(i, spot):
        for plan, unit in ((NEAR, near), (FAR, far)):
            begin, count, total = jnp.int32(0), jnp.int32(0), 0
            for n, counts in enumerate(plan):
                for at, units in zip((2, 0, 1), counts):
                    if at == spot:
                        begin = begin + jnp.where(i == n, total, 0)
                        count = count + jnp.where(i == n, units, 0)
                    total += units
            lax.fori_loop(begin, begin + count, unit, 0)

    def step(i, carry):
        attend(i, 2)
        first_half(i)
        for n in range(2):
            wide(i, n).start()

        @pl.when(i == LAST_AT)
        def _():
            for n in range(2):
                wide(ep - 1, n).start()

        @pl.when(i == EARLY_LAST)
        def _():
            first_half(ep - 1)

        @pl.when(i == NEAR_AT)
        def _():
            keys_out(1).wait_recv()
            keys_on(4, 1).wait_recv()

        @pl.when(i == FAR_AT)
        def _():
            keys_on(2, 1).wait_recv()
            keys_on(6, 1).wait_recv()


        attend(i, 0)
        @pl.when(i < ep - 2)
        def _():
            relay(i + 1)

        @pl.when(i < ep - 3)
        def _():
            enter(i + 2)

        @pl.when(i < ep - 5)
        def _():
            dispatch(i + 4).start()

        @pl.when(i == 1)
        def _():
            ret[0] = second_half(0)

        @pl.when(i > 1)
        def _():
            res[i - 1] = second_half(i - 1)
            back(i - 1).start()

        attend(i, 1)
        for n in range(2):
            wide(i, n).wait_recv()
            wide_on(i, n).start()

        @pl.when(i == NEAR_AT - 1)
        def _():
            keys_out(4).wait_recv()
            keys_on(4, 2).start()
            keys_on(4, 1).start()

        @pl.when(i == FAR_AT - 1)
        def _():
            keys_out(2).wait_recv()
            keys_on(2, 1).start()
            keys_on(4, 2).wait_recv()
            keys_on(6, 1).start()

        @pl.when(i == LAST_AT)
        def _():
            for n in range(2):
                wide(ep - 1, n).wait_recv()
                wide_on(ep - 1, n).start()
        return carry

    lax.fori_loop(0, ep - 1, step, 0)
    att_out = pltpu.make_async_copy(att_v, att_hbm, o_sem.at[0])
    att_out.start()

    def weighed(start, rows):
        block = ret[start : start + rows].reshape(rows * cap, chan)
        span = slice(start * cap, (start + rows) * cap)
        one = jnp.dot(pick0[:, span], block, preferred_element_type=f32)
        two = jnp.dot(pick1[:, span], block, preferred_element_type=f32)
        return mix_ref[:, 0:1] * one + mix_ref[:, 1:2] * two

    for p in range(1, ep - 3):
        back(p).wait_recv()
    acc[...] = weighed(0, ep - 3)
    res[ep - 1] = second_half(ep - 1)
    back(ep - 1).start()
    res[ep - 2] = second_half(ep - 2)
    back(ep - 2).start()
    back(ep - 3).wait_recv()
    acc[...] = acc[...] + weighed(ep - 3, 1)
    back(ep - 1).wait_recv()
    back(ep - 2).wait_recv()
    moe_v[...] = (acc[...] + weighed(ep - 2, 2)).astype(bf)
    moe_out = pltpu.make_async_copy(moe_v, moe_hbm, o_sem.at[1])
    moe_out.start()

    for p in range(ep):
        for n in range(2):
            cross(p, n).wait_send()
            cross_on(p, n).wait_send()
            wide(p, n).wait_send()
            wide_on(p, n).wait_send()
        if p > 0:
            dispatch(p).wait_send()
            back(p).wait_send()
    for j in (1, 2, 4):
        keys_out(j).wait_send()
    keys_on(4, 2).wait_send()
    for j in (2, 4, 6):
        keys_on(j, 1).wait_send()
    att_out.wait()
    moe_out.wait()


EARLY_LAST = 0
LAST_AT = 5
NEAR_AT = 1
FAR_AT = 3
NEAR = ((0, 0, 0), (0, 2, 1), (1, 2, 1), (1, 0, 0), (0, 0, 0), (0, 0, 0), (0, 0, 0))
FAR = ((0, 0, 0), (0, 0, 0), (0, 0, 0), (0, 1, 1), (1, 1, 1), (1, 1, 1), (0, 0, 0))


def angle_tables(lines):
    lane = np.arange(128)
    pair_count = HEAD_DIM // 4
    frequency = (10000.0 ** (-(lane % pair_count) / pair_count)).astype(np.float32)
    on_rows = (lane // (2 * pair_count)) % 2 == 0
    sign = np.where((lane // pair_count) % 2 == 0, -1.0, 1.0)

    def table(count, mine):
        angle = (np.arange(count, dtype=np.float32)[:, None] * frequency).astype(np.float64)
        both = np.concatenate(
            [np.cos(angle) * mine, np.sin(angle) * sign * mine], axis=1
        )
        return both.astype(np.float32)

    return table(lines, on_rows)[:, None, :], table(GRID_W, ~on_rows)


def on_device(
    queries, keys, values, query_gain, key_gain, moe_rows, route_ids, group_weight,
    expert_weight, expert_gate, expert_up, expert_down,
):
    ep, tp = lax.axis_size("ep"), lax.axis_size("tp")
    moe_tokens, chan = moe_rows.shape
    tok = queries.shape[0]
    cap = 3 * moe_tokens * TOPK // (2 * expert_gate.shape[0] * ep)
    fits = tp == 4 and ep == 8 and cap % 32 == 0 and expert_gate.shape[0] == 1
    fits = fits and tok == moe_tokens and tok % GRID_W == 0
    if not fits or queries.shape[1] // 128 != 8 or keys.shape[1] // 128 != 2:
        return plain_on_device(
            queries, keys, values, query_gain, key_gain, moe_rows, route_ids, group_weight,
            expert_weight, expert_gate, expert_up, expert_down,
        )
    rowtab, coltab = angle_tables(ep * tok // GRID_W)
    heads = queries.shape[1] // HEAD_DIM
    slabs = keys.shape[1] // 128
    width = expert_gate.shape[2]
    vmem = pl.BlockSpec(memory_space=pltpu.VMEM)
    hbm = pl.BlockSpec(memory_space=pl.ANY)
    dma = pltpu.SemaphoreType.DMA
    bf, f32 = jnp.bfloat16, jnp.float32
    attended, moe_out = pl.pallas_call(
        lambda *refs: main_kernel(ep, cap, *refs),
        out_shape=(
            jax.ShapeDtypeStruct(queries.shape, bf),
            jax.ShapeDtypeStruct(moe_rows.shape, bf),
        ),
        in_specs=[vmem] * 7 + [hbm] * 7,
        out_specs=(hbm, hbm),
        scratch_shapes=[
            pltpu.VMEM(moe_rows.shape, bf),
            pltpu.VMEM(keys.shape, bf),
            pltpu.VMEM(values.shape, bf),
            pltpu.VMEM(queries.shape, bf),
            pltpu.VMEM((ep, 1, tok), f32),
            pltpu.VMEM((tok, ep * cap), bf),
            pltpu.VMEM((tok, ep * cap), bf),
            pltpu.VMEM((tok, 8), f32),
            pltpu.VMEM((ep, cap, chan), bf),
            pltpu.VMEM((ep, tp, cap, chan), bf),
            pltpu.VMEM((ep, tp, cap, width), bf),
            pltpu.VMEM((ep, cap, chan), bf),
            pltpu.VMEM((ep, cap, chan), bf),
            pltpu.VMEM((ep, 2 * slabs, tok, 128), bf),
            pltpu.VMEM((heads, tok, 128), bf),
            pltpu.VMEM((heads, tok, 1), f32),
            pltpu.VMEM((heads, tok, 1), f32),
            pltpu.VMEM((heads, tok, 128), f32),
            pltpu.VMEM((tok, 128), f32),
            pltpu.VMEM((tok, 128), f32),
            pltpu.VMEM((tok, chan), f32),
            pltpu.VMEM(queries.shape, bf),
            pltpu.VMEM(moe_rows.shape, bf),
            pltpu.VMEM(expert_gate.shape[1:], bf),
            pltpu.VMEM(expert_up.shape[1:], bf),
            pltpu.VMEM(expert_down.shape[1:], bf),
            dma((7,)), dma((2,)), dma((ep,)), dma((ep,)),
            dma((ep, 2)), dma((ep, 2)), dma((ep, 2)), dma((ep, 2)),
            dma((ep, 2)), dma((ep, 2)), dma((ep, 2)), dma((ep, 2)),
            dma((ep,)), dma((ep,)), dma((ep,)), dma((ep,)),
        ],
        compiler_params=pltpu.CompilerParams(
            collective_id=0, has_side_effects=True, vmem_limit_bytes=60 * 1024 * 1024
        ),
    )(
        query_gain[None, :], key_gain[None, :], jnp.asarray(rowtab), jnp.asarray(coltab),
        route_ids.T, group_weight[None, :], expert_weight.T,
        moe_rows, keys, values, queries, expert_gate, expert_up, expert_down,
    )
    return (attended, moe_out)


def solution(mesh):
    placed = (
        P("ep", "tp"),
        P("ep", "tp"),
        P("ep", "tp"),
        P(),
        P(),
        P("ep", "tp"),
        P("ep", None),
        P("ep"),
        P("ep", None),
        P("ep", None, "tp"),
        P("ep", None, "tp"),
        P("ep", None, "tp"),
    )
    return jax.shard_map(
        on_device,
        mesh=mesh,
        in_specs=placed,
        out_specs=(P("ep", "tp"), P("ep", "tp")),
        check_vma=False,
    )
```

```python
import jax
import jax.numpy as jnp
import numpy as np
from jax import lax
from jax.experimental import pallas as pl
from jax.experimental.pallas import tpu as pltpu
from jax.sharding import PartitionSpec as P

D = 4096
HEAD_DIM = 64
GRID_W = 64
TOPK = 2


def rotary_tables(position):
    pair_count = HEAD_DIM // 4
    grid_pos = jnp.stack([position // GRID_W, position % GRID_W], axis=-1).astype(jnp.float32)
    frequency = 10000.0 ** (-jnp.arange(pair_count, dtype=jnp.float32) / pair_count)
    angles = grid_pos[:, :, None] * frequency
    return (jnp.cos(angles), jnp.sin(angles))


def normed_rotated(rows_in, gain, cosine, sine_of):
    row_count, head_count = (rows_in.shape[0], rows_in.shape[1])
    pair_count = HEAD_DIM // 4
    scaled = rows_in * lax.rsqrt(jnp.mean(rows_in * rows_in, axis=-1, keepdims=True) + 1e-06) * gain
    parted = scaled.reshape(row_count, head_count, 2, 2, pair_count)
    first_half, second = (parted[:, :, :, 0, :], parted[:, :, :, 1, :])
    cos_b, sin_b = (cosine[:, None], sine_of[:, None])
    turned = jnp.stack(
        [first_half * cos_b - second * sin_b, second * cos_b + first_half * sin_b], axis=3
    )
    return turned.reshape(row_count, head_count, HEAD_DIM).astype(jnp.bfloat16)


def attend_block(carried, portion, query_rot, kv_width):
    running_max, denominator, summed = carried
    key_count = portion.shape[0]
    head_count = kv_width // HEAD_DIM
    keys_part = portion[:, :kv_width].reshape(key_count, head_count, HEAD_DIM)
    values_part = portion[:, kv_width:].reshape(key_count, head_count, HEAD_DIM)
    scores = jnp.einsum(
        "tkgd,skd->kgts", query_rot, keys_part, preferred_element_type=jnp.float32
    ) * HEAD_DIM ** (-0.5)
    new_max = jnp.max(scores, axis=-1)
    factor = jnp.exp(running_max - new_max)
    weights = jnp.exp(scores - new_max[..., None])
    denominator = denominator * factor + jnp.sum(weights, axis=-1)
    summed = summed * factor[..., None] + jnp.einsum(
        "kgts,skd->kgtd",
        weights.astype(jnp.bfloat16),
        values_part,
        preferred_element_type=jnp.float32,
    )
    return (new_max, denominator, summed)


def plain_on_device(
    queries,
    keys,
    values,
    query_gain,
    key_gain,
    moe_rows,
    route_ids,
    group_weight,
    expert_weight,
    expert_gate,
    expert_up,
    expert_down,
):
    tok_rows = queries.shape[0]
    q_heads = queries.shape[1] // HEAD_DIM
    k_heads = keys.shape[1] // HEAD_DIM
    group_size = q_heads // k_heads
    position = lax.axis_index("ep") * tok_rows + jnp.arange(tok_rows, dtype=jnp.int32)
    cosine, sine_of = rotary_tables(position)
    query_rot = normed_rotated(
        queries.astype(jnp.float32).reshape(tok_rows, q_heads, HEAD_DIM),
        query_gain,
        cosine,
        sine_of,
    )
    query_rot = query_rot.reshape(tok_rows, k_heads, group_size, HEAD_DIM)
    key_rot = normed_rotated(
        keys.astype(jnp.float32).reshape(tok_rows, k_heads, HEAD_DIM), key_gain, cosine, sine_of
    )
    kv_width = k_heads * HEAD_DIM
    joined = jnp.concatenate([key_rot.reshape(tok_rows, kv_width), values], axis=1)
    initial = (
        jnp.full((k_heads, group_size, tok_rows), -jnp.inf, jnp.float32),
        jnp.zeros((k_heads, group_size, tok_rows), jnp.float32),
        jnp.zeros((k_heads, group_size, tok_rows, HEAD_DIM), jnp.float32),
    )
    final_max, denominator, summed = attend_block(
        initial, lax.all_gather(joined, "ep", axis=0, tiled=True), query_rot, kv_width
    )
    attended = (
        (summed / denominator[..., None])
        .transpose(2, 0, 1, 3)
        .reshape(tok_rows, q_heads * HEAD_DIM)
        .astype(jnp.bfloat16)
    )
    moe_tokens = moe_rows.shape[0]
    local_experts = expert_gate.shape[0]
    expert_count = local_experts * lax.axis_size("ep")
    capacity = 3 * moe_tokens * TOPK // (2 * expert_count)
    picks = moe_tokens * TOPK
    route_list = route_ids.reshape(picks)
    one_hot = (route_list[:, None] == jnp.arange(expert_count, dtype=jnp.int32)[None, :]).astype(
        jnp.int32
    )
    rank_of = jnp.sum((jnp.cumsum(one_hot, axis=0) - one_hot) * one_hot, axis=1)
    slot_of = route_list * capacity + rank_of
    owner_of = (
        jnp.full((expert_count * capacity,), moe_tokens, jnp.int32)
        .at[slot_of]
        .set(jnp.arange(picks, dtype=jnp.int32) // TOPK)
    )
    padded = jnp.concatenate([moe_rows, jnp.zeros((1, moe_rows.shape[1]), moe_rows.dtype)], axis=0)
    arrived = lax.all_to_all(
        padded[owner_of].reshape(expert_count, capacity, moe_rows.shape[1]),
        "ep",
        split_axis=0,
        concat_axis=1,
        tiled=True,
    )
    portion = lax.all_gather(arrived, "tp", axis=2, tiled=True)
    widened = portion.astype(jnp.float32)
    gate_act = jnp.einsum("erd,edf->erf", portion, expert_gate, preferred_element_type=jnp.float32)
    up_act = jnp.einsum("erd,edf->erf", portion, expert_up, preferred_element_type=jnp.float32)
    square_sum = jnp.sum(widened * widened, axis=2)
    inv_rms = lax.rsqrt(square_sum / D + 1e-06)[..., None]
    hidden = (jax.nn.silu(gate_act * inv_rms) * (up_act * inv_rms)).astype(jnp.bfloat16)
    out_cols = expert_down.shape[2]
    expert_result = jnp.einsum(
        "erf,efd->erd",
        lax.all_gather(hidden, "tp", axis=2, tiled=True),
        expert_down,
        preferred_element_type=jnp.float32,
    ).astype(jnp.bfloat16)
    returned = lax.all_to_all(expert_result, "ep", split_axis=1, concat_axis=0, tiled=True)
    flat_back = returned.reshape(expert_count * capacity, out_cols)
    picked = flat_back[slot_of].reshape(moe_tokens, TOPK, out_cols).astype(jnp.float32)
    mixing = group_weight[:, None] * expert_weight / jnp.sum(expert_weight, axis=1, keepdims=True)
    moe_out = jnp.sum(mixing[:, :, None] * picked, axis=1).astype(jnp.bfloat16)
    return (attended, moe_out)


MESH = pl.DeviceIdType.MESH


def flip(index, mask, width):
    out = 0
    bit = 1
    while bit < width:
        a, b = (index // bit) % 2, (mask // bit) % 2
        out = out + bit * (a + b - 2 * a * b)
        bit *= 2
    return out


def sub_iota(shape):
    return lax.broadcasted_iota(jnp.int32, shape, 0)


def lane_iota(shape):
    return lax.broadcasted_iota(jnp.int32, shape, 1)


def main_kernel(
    ep, cap,
    qg_ref, kg_ref, rowtab, coltab, route_ref, gw_ref, ew_ref,
    rows_hbm, k_hbm, v_hbm, q_hbm, wg_hbm, wu_hbm, wd_hbm,
    att_hbm, moe_hbm,
    rows_v, k_v, v_v, q_v, code_ref, pick0, pick1, mix_ref, picks,
    xg, hid, res, ret, kvall, q_s, tops, dens, part_o, cos_ref, sin_ref, acc, att_v, moe_v, wg, wu, wd,
    l_sem, o_sem, d_send, d_recv, x_send, x_recv, xr_send, xr_recv,
    h_send, h_recv, hr_send, hr_recv, r_send, r_recv, k_send, k_recv,
):
    me, tme = lax.axis_index("ep"), lax.axis_index("tp")
    sides = (flip(tme, 1, 4), flip(tme, 2, 4))
    half = cap // 2
    width = wg.shape[1]
    tok, chan = rows_v.shape
    f32, bf = jnp.float32, jnp.bfloat16
    order = (0, *range(2, ep), 1)

    def mask(p):
        if isinstance(p, int):
            return order[p]
        return jnp.where(p == 0, 0, p % (ep - 1) + 1)

    def peer(p):
        return flip(me, mask(p), ep)

    pairs = (
        (rows_hbm, rows_v), (k_hbm, k_v), (v_hbm, v_v), (q_hbm, q_v),
        (wg_hbm.at[0], wg), (wu_hbm.at[0], wu), (wd_hbm.at[0], wd),
    )
    loads = [pltpu.make_async_copy(a, b, l_sem.at[n]) for n, (a, b) in enumerate(pairs)]
    for copy in loads:
        copy.start()
    barrier = pltpu.get_barrier_semaphore()
    for j in range(1, ep):
        pl.semaphore_signal(barrier, inc=1, device_id={"ep": flip(me, j, ep)}, device_id_type=MESH)
    for side in sides:
        pl.semaphore_signal(barrier, inc=1, device_id={"tp": side}, device_id_type=MESH)

    def remote(src, dst, send, recv, device):
        return pltpu.make_async_remote_copy(
            src_ref=src, dst_ref=dst, send_sem=send, recv_sem=recv,
            device_id=device, device_id_type=MESH,
        )

    def dispatch(p):
        return remote(picks.at[p], xg.at[p, tme], d_send.at[p], d_recv.at[p], {"ep": peer(p)})

    def slot(b):
        return b // 2 % 2 * (ep // 2) + b // 4 * 2 + b % 2

    def keys_out(j):
        part = kvall.at[slot(me)]
        return remote(
            part, part, k_send.at[j], k_recv.at[j], {"ep": flip(me, j, ep)}
        )

    def keys_on(j, to):
        part = kvall.at[slot(flip(me, j, ep))]
        n = flip(j, to, ep)
        return remote(
            part, part, k_send.at[n], k_recv.at[n],
            {"ep": flip(me, to, ep)},
        )

    def cross(p, n):
        part = xg.at[p, tme]
        return remote(part, part, x_send.at[p, n], x_recv.at[p, n], {"tp": sides[n]})

    def cross_on(p, n):
        part = xg.at[p, sides[n], pl.ds(n * half, half)]
        return remote(part, part, xr_send.at[p, n], xr_recv.at[p, n], {"tp": sides[1 - n]})

    def wide(p, n):
        part = hid.at[p, tme]
        return remote(part, part, h_send.at[p, n], h_recv.at[p, n], {"tp": sides[n]})

    def wide_on(p, n):
        part = hid.at[p, sides[n], pl.ds(n * half, half)]
        return remote(part, part, hr_send.at[p, n], hr_recv.at[p, n], {"tp": sides[1 - n]})

    def back(p):
        return remote(res.at[p], ret.at[p], r_send.at[p], r_recv.at[p], {"ep": peer(p)})

    experts = sub_iota((16, tok))
    first = route_ref[0:1, :] == experts
    second = route_ref[1:2, :] == experts
    both = jnp.logical_or(first, second)
    earlier = jnp.where(sub_iota((tok, tok)) < lane_iota((tok, tok)), 1.0, 0.0).astype(bf)
    rank = jnp.dot(
        jnp.where(both, 1.0, 0.0).astype(bf), earlier, preferred_element_type=f32
    )
    code = jnp.where(both, rank, -1.0)
    for e in range(ep):
        code_ref[e] = code[e : e + 1, :]
    slots = sub_iota((cap, tok)).astype(f32)

    def select(p):
        chosen = jnp.where(code_ref[peer(p)] == slots, 1.0, 0.0).astype(bf)
        return jnp.dot(chosen, rows_v[...], preferred_element_type=f32).astype(bf)

    loads[0].wait()
    xg[0, tme] = select(0)
    picks[1] = select(1)
    pl.semaphore_wait(barrier, ep + 1)
    for n in range(2):
        cross(0, n).start()
    dispatch(1).start()
    picks[ep - 1] = select(ep - 1)
    dispatch(ep - 1).start()

    def enter(p):
        dispatch(p).wait_recv()
        for n in range(2):
            cross(p, n).start()

    def relay(p):
        for n in range(2):
            cross(p, n).wait_recv()
            cross_on(p, n).start()

    picks[2] = select(2)
    spread = jnp.where(
        sub_iota((128, 128)) // HEAD_DIM == lane_iota((128, 128)) // HEAD_DIM, 1.0 / HEAD_DIM, 0.0
    ).astype(f32)
    grid_rows = tok // GRID_W
    for g in range(grid_rows):
        line = rowtab[me * grid_rows + g]
        cos_ref[g * GRID_W : (g + 1) * GRID_W, :] = line[:, :128] + coltab[:, :128]
        sin_ref[g * GRID_W : (g + 1) * GRID_W, :] = line[:, 128:] + coltab[:, 128:]
    lane = lane_iota((tok, 128))
    half_one = lane % 32 < 16
    low = lane < HEAD_DIM

    def turned(x, gain):
        x = x.astype(f32)
        mean = jnp.dot(
            x * x, spread, preferred_element_type=f32, precision=lax.Precision.HIGHEST
        )
        y = x * lax.rsqrt(mean + 1e-06) * gain
        partner = jnp.where(half_one, pltpu.roll(y, 112, 1), pltpu.roll(y, 16, 1))
        return y * cos_ref[...] + partner * sin_ref[...]

    q_gain = jnp.concatenate([qg_ref[...], qg_ref[...]], axis=1)
    k_gain = jnp.concatenate([kg_ref[...], kg_ref[...]], axis=1)
    k_slabs = k_v.shape[1] // 128
    slabs = q_v.shape[1] // 128
    per_kv = slabs // (2 * k_slabs)
    loads[1].wait()
    loads[2].wait()
    for s in range(k_slabs):
        kvall[slot(me), s] = turned(k_v[:, s * 128 : (s + 1) * 128], k_gain).astype(bf)
        kvall[slot(me), k_slabs + s] = v_v[:, s * 128 : (s + 1) * 128]
    for j in (1, 4):
        keys_out(j).start()
    enter(ep - 1)
    for p in range(3, ep - 1):
        picks[p] = select(p)
    relay(0)
    dispatch(2).start()
    enter(1)
    relay(ep - 1)
    dispatch(3).start()

    loads[3].wait()
    for s in range(slabs):
        r = turned(q_v[:, s * 128 : (s + 1) * 128], q_gain)
        r = r.astype(bf).astype(f32) * HEAD_DIM ** (-0.5)
        moved = pltpu.roll(r, HEAD_DIM, 1)
        if (s // per_kv) % 2 == 0:
            pair = (jnp.where(low, r, 0.0), jnp.where(low, moved, 0.0))
        else:
            pair = (jnp.where(low, 0.0, moved), jnp.where(low, 0.0, r))
        q_s[2 * s] = pair[0].astype(bf)
        q_s[2 * s + 1] = pair[1].astype(bf)

    columns = lane_iota((16, ep * cap))
    place = jnp.zeros((16, ep * cap), jnp.int32)
    for n in range(1, ep):
        place = place + jnp.where(columns >= n * cap, 1, 0)
    xor_of = jnp.zeros((16, ep * cap), jnp.int32)
    for n in range(ep):
        xor_of = xor_of + jnp.where(place == n, order[n], 0)
    named = jnp.where(sub_iota((16, ep * cap)) == jnp.bitwise_xor(xor_of, me), 1.0, 0.0).astype(bf)
    rest = (columns - place * cap).astype(f32)[0:1, :]
    for wanted, out in ((first, pick0), (second, pick1)):
        of_token = jnp.where(wanted, rank, -1.0).T.astype(bf)
        spot = jnp.dot(of_token, named, preferred_element_type=f32)
        out[...] = jnp.where(spot == rest, 1.0, 0.0).astype(bf)
    weight = gw_ref[...] * ew_ref[...] / jnp.sum(ew_ref[...], axis=0, keepdims=True)
    mix_ref[...] = jnp.concatenate([weight, jnp.zeros((6, tok), f32)], axis=0).T

    keys_out(2).start()
    for copy in loads[4:]:
        copy.wait()

    def first_half(p):
        for n in range(2):
            cross_on(p, n).wait_recv()
        gate = jnp.zeros((cap, width), f32)
        up = jnp.zeros((cap, width), f32)
        square = jnp.zeros((cap, 1), f32)
        for a in range(4):
            x = xg[p, a]
            w = x.astype(f32)
            square = square + jnp.sum(w * w, axis=1, keepdims=True)
            gate = gate + jnp.dot(x, wg[a * chan : (a + 1) * chan, :], preferred_element_type=f32)
            up = up + jnp.dot(x, wu[a * chan : (a + 1) * chan, :], preferred_element_type=f32)
        inv = lax.rsqrt(square / D + 1e-06)
        g = gate * inv
        hid[p, tme] = (g / (1.0 + jnp.exp(-g)) * (up * inv)).astype(bf)

    def second_half(p):
        for n in range(2):
            wide_on(p, n).wait_recv()
        total = jnp.zeros((cap, chan), f32)
        for a in range(4):
            total = total + jnp.dot(
                hid[p, a], wd[a * width : (a + 1) * width, :], preferred_element_type=f32
            )
        return total.astype(bf)

    keys_total = ep * tok

    part_keys = keys_total // 2

    def scores(m, d, group):
        pp = m // (2 * per_kv)
        blocks = pl.ds(group * (ep // 2), ep // 2)
        k = kvall[blocks, pp].reshape(part_keys, 128)
        v = kvall[blocks, k_slabs + pp].reshape(part_keys, 128)
        s = lax.dot_general(
            q_s[2 * m + d], k, (((1,), (1,)), ((), ())), preferred_element_type=f32
        )
        return s, v

    def near(m, carry):
        for d in range(2):
            s, v = scores(m, d, me // 2 % 2)
            top = jnp.max(s, axis=1, keepdims=True)
            p = jnp.exp(s - top)
            tops[2 * m + d] = top
            dens[2 * m + d] = jnp.sum(p, axis=1, keepdims=True)
            part_o[2 * m + d] = jnp.dot(p.astype(bf), v, preferred_element_type=f32)
        return carry

    def far(m, carry):
        outs = []
        for d in range(2):
            s, v = scores(m, d, 1 - me // 2 % 2)
            before = tops[2 * m + d]
            top = jnp.maximum(before, jnp.max(s, axis=1, keepdims=True))
            scale = jnp.exp(before - top)
            p = jnp.exp(s - top)
            den = dens[2 * m + d] * scale + jnp.sum(p, axis=1, keepdims=True)
            o = part_o[2 * m + d] * scale + jnp.dot(p.astype(bf), v, preferred_element_type=f32)
            outs.append(o / den)
        even = jnp.where(low, outs[0], pltpu.roll(outs[1], HEAD_DIM, 1))
        odd = jnp.where(low, pltpu.roll(outs[0], HEAD_DIM, 1), outs[1])
        side = ((m // per_kv) % 2).astype(f32)
        joined = jnp.where(side == 0.0, even, odd)
        att_v[:, pl.ds(pl.multiple_of(m * 128, 128), 128)] = joined.astype(bf)
        return carry

    def attend(i, spot):
        for plan, unit in ((NEAR, near), (FAR, far)):
            begin, count, total = jnp.int32(0), jnp.int32(0), 0
            for n, counts in enumerate(plan):
                for at, units in zip((2, 0, 1), counts):
                    if at == spot:
                        begin = begin + jnp.where(i == n, total, 0)
                        count = count + jnp.where(i == n, units, 0)
                    total += units
            lax.fori_loop(begin, begin + count, unit, 0)

    def step(i, carry):
        attend(i, 2)
        first_half(i)
        for n in range(2):
            wide(i, n).start()

        @pl.when(i == LAST_AT)
        def _():
            for n in range(2):
                wide(ep - 1, n).start()

        @pl.when(i == LAST_AT + 1)
        def _():
            for n in range(2):
                wide(ep - 1, n).wait_recv()
                wide_on(ep - 1, n).start()

        @pl.when(i == NEAR_AT)
        def _():
            keys_out(1).wait_recv()
            keys_on(4, 1).wait_recv()

        @pl.when(i == FAR_AT)
        def _():
            keys_on(2, 1).wait_recv()
            keys_on(6, 1).wait_recv()


        attend(i, 0)
        @pl.when(i < ep - 2)
        def _():
            relay(i + 1)

        @pl.when(i < ep - 3)
        def _():
            enter(i + 2)

        @pl.when(i < ep - 5)
        def _():
            dispatch(i + 4).start()

        @pl.when(i == EARLY_LAST)
        def _():
            first_half(ep - 1)

        @pl.when(i == 1)
        def _():
            ret[0] = second_half(0)

        @pl.when(i > 1)
        def _():
            res[i - 1] = second_half(i - 1)
            back(i - 1).start()

        attend(i, 1)
        for n in range(2):
            wide(i, n).wait_recv()
            wide_on(i, n).start()

        @pl.when(i == NEAR_AT - 1)
        def _():
            keys_out(4).wait_recv()
            keys_on(4, 2).start()
            keys_on(4, 1).start()

        @pl.when(i == FAR_AT - 1)
        def _():
            keys_out(2).wait_recv()
            keys_on(2, 1).start()
            keys_on(4, 2).wait_recv()
            keys_on(6, 1).start()

        return carry

    lax.fori_loop(0, ep - 1, step, 0)
    att_out = pltpu.make_async_copy(att_v, att_hbm, o_sem.at[0])
    att_out.start()

    def weighed(start, rows):
        block = ret[start : start + rows].reshape(rows * cap, chan)
        span = slice(start * cap, (start + rows) * cap)
        one = jnp.dot(pick0[:, span], block, preferred_element_type=f32)
        two = jnp.dot(pick1[:, span], block, preferred_element_type=f32)
        return mix_ref[:, 0:1] * one + mix_ref[:, 1:2] * two

    for p in range(1, ep - 3):
        back(p).wait_recv()
    acc[...] = weighed(0, ep - 3)
    res[ep - 1] = second_half(ep - 1)
    back(ep - 1).start()
    res[ep - 2] = second_half(ep - 2)
    back(ep - 2).start()
    back(ep - 3).wait_recv()
    acc[...] = acc[...] + weighed(ep - 3, 1)
    back(ep - 1).wait_recv()
    back(ep - 2).wait_recv()
    moe_v[...] = (acc[...] + weighed(ep - 2, 2)).astype(bf)
    moe_out = pltpu.make_async_copy(moe_v, moe_hbm, o_sem.at[1])
    moe_out.start()

    for p in range(ep):
        for n in range(2):
            cross(p, n).wait_send()
            cross_on(p, n).wait_send()
            wide(p, n).wait_send()
            wide_on(p, n).wait_send()
        if p > 0:
            dispatch(p).wait_send()
            back(p).wait_send()
    for j in (1, 2, 4):
        keys_out(j).wait_send()
    keys_on(4, 2).wait_send()
    for j in (2, 4, 6):
        keys_on(j, 1).wait_send()
    att_out.wait()
    moe_out.wait()


def copy_kernel(att_in, moe_in, att_out, moe_out, held, in_sem, out_sem):
    rows = held.shape[1]
    parts = []
    for src, dst in ((att_in, att_out), (moe_in, moe_out)):
        for at in range(src.shape[0] // rows):
            span = pl.ds(at * rows, rows)
            n = len(parts)
            parts.append((
                pltpu.make_async_copy(src.at[span], held.at[n], in_sem.at[n]),
                pltpu.make_async_copy(held.at[n], dst.at[span], out_sem.at[n]),
            ))
    for into, _ in parts:
        into.start()
    for into, out in parts:
        into.wait()
        out.start()
    for _, out in parts:
        out.wait()

EARLY_LAST = 0
NEAR_AT = 1
FAR_AT = 3
NEAR = ((0, 0, 0), (0, 2, 1), (1, 2, 1), (1, 0, 0), (0, 0, 0), (0, 0, 0), (0, 0, 0))
LAST_AT = 5
FAR = ((0, 0, 0), (0, 0, 0), (0, 0, 0), (0, 2, 1), (1, 2, 1), (0, 1, 0), (0, 0, 0))


def angle_tables(lines):
    lane = np.arange(128)
    pair_count = HEAD_DIM // 4
    frequency = (10000.0 ** (-(lane % pair_count) / pair_count)).astype(np.float32)
    on_rows = (lane // (2 * pair_count)) % 2 == 0
    sign = np.where((lane // pair_count) % 2 == 0, -1.0, 1.0)

    def table(count, mine):
        angle = (np.arange(count, dtype=np.float32)[:, None] * frequency).astype(np.float64)
        both = np.concatenate(
            [np.cos(angle) * mine, np.sin(angle) * sign * mine], axis=1
        )
        return both.astype(np.float32)

    return table(lines, on_rows)[:, None, :], table(GRID_W, ~on_rows)


def on_device(
    queries, keys, values, query_gain, key_gain, moe_rows, route_ids, group_weight,
    expert_weight, expert_gate, expert_up, expert_down,
):
    ep, tp = lax.axis_size("ep"), lax.axis_size("tp")
    moe_tokens, chan = moe_rows.shape
    tok = queries.shape[0]
    cap = 3 * moe_tokens * TOPK // (2 * expert_gate.shape[0] * ep)
    fits = tp == 4 and ep == 8 and cap % 32 == 0 and expert_gate.shape[0] == 1
    fits = fits and tok == moe_tokens and tok % GRID_W == 0
    if not fits or queries.shape[1] // 128 != 8 or keys.shape[1] // 128 != 2:
        return plain_on_device(
            queries, keys, values, query_gain, key_gain, moe_rows, route_ids, group_weight,
            expert_weight, expert_gate, expert_up, expert_down,
        )
    rowtab, coltab = angle_tables(ep * tok // GRID_W)
    heads = queries.shape[1] // HEAD_DIM
    slabs = keys.shape[1] // 128
    width = expert_gate.shape[2]
    vmem = pl.BlockSpec(memory_space=pltpu.VMEM)
    hbm = pl.BlockSpec(memory_space=pl.ANY)
    dma = pltpu.SemaphoreType.DMA
    bf, f32 = jnp.bfloat16, jnp.float32
    attended, moe_out = pl.pallas_call(
        lambda *refs: main_kernel(ep, cap, *refs),
        out_shape=(
            jax.ShapeDtypeStruct(queries.shape, bf),
            jax.ShapeDtypeStruct(moe_rows.shape, bf),
        ),
        in_specs=[vmem] * 7 + [hbm] * 7,
        out_specs=(hbm, hbm),
        scratch_shapes=[
            pltpu.VMEM(moe_rows.shape, bf),
            pltpu.VMEM(keys.shape, bf),
            pltpu.VMEM(values.shape, bf),
            pltpu.VMEM(queries.shape, bf),
            pltpu.VMEM((ep, 1, tok), f32),
            pltpu.VMEM((tok, ep * cap), bf),
            pltpu.VMEM((tok, ep * cap), bf),
            pltpu.VMEM((tok, 8), f32),
            pltpu.VMEM((ep, cap, chan), bf),
            pltpu.VMEM((ep, tp, cap, chan), bf),
            pltpu.VMEM((ep, tp, cap, width), bf),
            pltpu.VMEM((ep, cap, chan), bf),
            pltpu.VMEM((ep, cap, chan), bf),
            pltpu.VMEM((ep, 2 * slabs, tok, 128), bf),
            pltpu.VMEM((heads, tok, 128), bf),
            pltpu.VMEM((heads, tok, 1), f32),
            pltpu.VMEM((heads, tok, 1), f32),
            pltpu.VMEM((heads, tok, 128), f32),
            pltpu.VMEM((tok, 128), f32),
            pltpu.VMEM((tok, 128), f32),
            pltpu.VMEM((tok, chan), f32),
            pltpu.VMEM(queries.shape, bf),
            pltpu.VMEM(moe_rows.shape, bf),
            pltpu.VMEM(expert_gate.shape[1:], bf),
            pltpu.VMEM(expert_up.shape[1:], bf),
            pltpu.VMEM(expert_down.shape[1:], bf),
            dma((7,)), dma((2,)), dma((ep,)), dma((ep,)),
            dma((ep, 2)), dma((ep, 2)), dma((ep, 2)), dma((ep, 2)),
            dma((ep, 2)), dma((ep, 2)), dma((ep, 2)), dma((ep, 2)),
            dma((ep,)), dma((ep,)), dma((ep,)), dma((ep,)),
        ],
        compiler_params=pltpu.CompilerParams(
            collective_id=0, has_side_effects=True, vmem_limit_bytes=60 * 1024 * 1024
        ),
    )(
        query_gain[None, :], key_gain[None, :], jnp.asarray(rowtab), jnp.asarray(coltab),
        route_ids.T, group_weight[None, :], expert_weight.T,
        moe_rows, keys, values, queries, expert_gate, expert_up, expert_down,
    )
    return pl.pallas_call(
        copy_kernel,
        out_shape=(
            jax.ShapeDtypeStruct(queries.shape, bf),
            jax.ShapeDtypeStruct(moe_rows.shape, bf),
        ),
        in_specs=[hbm] * 2,
        out_specs=(hbm, hbm),
        scratch_shapes=[pltpu.VMEM((4, tok // 2, chan), bf), dma((4,)), dma((4,))],
    )(attended, moe_out)


def solution(mesh):
    placed = (
        P("ep", "tp"),
        P("ep", "tp"),
        P("ep", "tp"),
        P(),
        P(),
        P("ep", "tp"),
        P("ep", None),
        P("ep"),
        P("ep", None),
        P("ep", None, "tp"),
        P("ep", None, "tp"),
        P("ep", None, "tp"),
    )
    return jax.shard_map(
        on_device,
        mesh=mesh,
        in_specs=placed,
        out_specs=(P("ep", "tp"), P("ep", "tp")),
        check_vma=False,
    )
```
